32 devices in a mesh: fs: 4 (over y, x), tp: 8 (over z, core).
Axes of the slice: x: 2, y: 2, z: 4, core: 2. Of those that a mesh axis runs over, the one named last changes fastest.
Arguments:
- hidden_in: bfloat16 [6144, 4096], P('fs', 'tp'), may hold values from -6 to 6
- forget_pre: bfloat16 [6144, 2048], P('fs', 'tp'), may hold values from -8 to 8
- forget_cot: bfloat16 [6144, 2048], P('fs', 'tp'), may hold values from -0.4375 to 0.4375
- lower_bound: float32 [2048], P('tp'), may hold values from 0.05 to 0.9
- head_out: bfloat16 [6144, 2048], P('fs', 'tp'), may hold values from -6 to 6
- out_cot: bfloat16 [6144, 4096], P('fs', 'tp'), may hold values from -0.109375 to 0.109375
- basis_forget: bfloat16 [2048, 256], replicated, may hold values from -0.37565048 to 0.37565048
- basis_output: bfloat16 [2048, 256], replicated, may hold values from -0.37565048 to 0.37565048
- weight_forget: float32 [2048, 4096], P('fs', 'tp'), may hold values from -0.09375 to 0.09375
- weight_output: float32 [4096, 2048], P('tp', 'fs'), may hold values from -0.125 to 0.125
- mean_forget: float32 [256, 4096], P('fs', 'tp'), may hold values from -3.5 to 3.5
- var_forget: float32 [256, 4096], P('fs', 'tp'), may hold values from 0.003 to 0.05
- mean_output: float32 [256, 4096], P('fs', 'tp'), may hold values from -3.5 to 3.5
- var_output: float32 [256, 4096], P('fs', 'tp'), may hold values from 0.003 to 0.05
Outputs:
- step_forget: float32 [2048, 4096], P('fs', 'tp')
- step_output: float32 [4096, 2048], P('tp', 'fs')
- new_forget: float32 [2048, 4096], P('fs', 'tp')
- new_output: float32 [4096, 2048], P('tp', 'fs')
- mean_forget_new: float32 [256, 4096], P('fs', 'tp')
- var_forget_new: float32 [256, 4096], P('fs', 'tp')
- mean_output_new: float32 [256, 4096], P('fs', 'tp')
- var_output_new: float32 [256, 4096], P('fs', 'tp')
- copy_forget: bfloat16 [2048, 4096], P(None, 'tp')
- copy_output: bfloat16 [4096, 2048], P('tp')
The draws below stay inside these ranges and needn't reach their ends.
All inputs are finite; a program needn't handle non-finite values.
Results may differ from the reference program's by a relative error of at most 0.014.
Values may be sent and summed in bfloat16 or wider, within the bound.
A program may use at most 64 MiB of HBM per device.

```python
import math
import jax
import jax.numpy as jnp
from jax import lax

D = 4096
HW = 2048
RANK = 256
TOKENS = 6144


def rising_basis(key):
    position = jnp.arange(HW, dtype=jnp.float32) / HW
    rank_pos = jnp.arange(RANK, dtype=jnp.int32)
    first_group = rank_pos < RANK // 16
    second_group = (rank_pos >= RANK // 2 - RANK // 32) & (rank_pos < RANK // 2 + RANK // 32)
    grouped = first_group | second_group
    noise = jnp.clip(jax.random.normal(key, (HW, RANK), jnp.float32), -4.0, 4.0)
    common = jnp.clip(jax.random.normal(jax.random.fold_in(key, 21), (HW, 1), jnp.float32), -4.0, 4.0)
    scale = jnp.exp(jnp.log(4.0) * position)
    mixed = jnp.where(grouped[None, :], 0.7 * noise + 0.7 * common, noise)
    value = jnp.clip(mixed * scale[:, None], -16.5, 16.5)
    return (value * HW ** (-0.5)).astype(jnp.bfloat16)


def rising_moment(key):
    position = jnp.arange(D, dtype=jnp.float32) / D
    scale = 0.2 * jnp.exp(jnp.log(4.0) * position)
    first = jax.random.normal(jax.random.fold_in(key, 5), (RANK, D), jnp.float32)
    noise = jnp.clip(first, -4.0, 4.0)
    return noise * scale[None, :]


def draw_basis_forget(key, part):
    return rising_basis(jax.random.fold_in(key, 11))


def draw_basis_output(key, part):
    return rising_basis(jax.random.fold_in(key, 12))


def draw_mean_forget(key, part):
    return rising_moment(jax.random.fold_in(key, 13))


def draw_mean_output(key, part):
    return rising_moment(jax.random.fold_in(key, 14))


def steps_of(key, dims, split, low, high):
    def one(dim, shards_of):
        draws = jax.random.uniform(jax.random.fold_in(jax.random.fold_in(key, 6), dim), (shards_of,), jnp.float32, low / len(split), high / len(split))
        return jnp.repeat(jnp.exp(draws), dims[dim] // shards_of).reshape((-1,) + (1,) * (len(dims) - dim - 1))

    loudness = one(*split[0])
    for cut in split[1:]:
        loudness = loudness * one(*cut)
    return loudness


def bell_draw(rng, shape, scale, limit, pieces=(), kind=jnp.bfloat16):
    array = jax.random.normal(rng, shape, jnp.float32) * scale
    if len(pieces) > 0:
        array = steps_of(rng, shape, pieces, -0.22, 0.18) * array
    return jnp.clip(array, min=-limit, max=limit).astype(kind)


def setup_inputs(seed: int = 0) -> dict:
    key_list = jax.random.split(jax.random.key(seed), 15)
    hidden_in = bell_draw(key_list[0], (TOKENS, D), 1.0, 6.0, ((0, 4), (1, 8)))
    forget_pre = bell_draw(key_list[1], (TOKENS, HW), 1.5, 8.0, ((0, 4), (1, 8)))
    forget_cot = bell_draw(key_list[2], (TOKENS, HW), (6 / TOKENS ** 0.5), 0.4375, ((0, 4), (1, 8)))
    lower_bound = jnp.clip(0.05 + 0.84999998 * jax.random.uniform(key_list[3], (HW,), jnp.float32) ** steps_of(key_list[3], (HW,), ((0, 8),), -0.2, 0.2), 0.05, 0.9)
    head_out = bell_draw(key_list[4], (TOKENS, HW), 1.0, 6.0, ((0, 4), (1, 8)))
    out_cot = bell_draw(key_list[5], (TOKENS, D), (1.5 / TOKENS ** 0.5), 0.109375, ((0, 4), (1, 8)))
    basis_forget = draw_basis_forget(jax.random.fold_in(key_list[14], 71), 0)
    basis_output = draw_basis_output(jax.random.fold_in(key_list[14], 71), 0)
    weight_forget = bell_draw(key_list[8], (HW, D), D ** -0.5, 0.09375, ((0, 4), (1, 8)), jnp.float32)
    weight_output = bell_draw(key_list[9], (D, HW), HW ** -0.5, 0.125, ((0, 8), (1, 4)), jnp.float32)
    mean_forget = draw_mean_forget(jax.random.fold_in(key_list[14], 71), 0)
    var_forget = jnp.clip(jnp.exp(math.log(0.05) - 2.8134107 * jax.random.uniform(key_list[11], (RANK, D), jnp.float32) ** steps_of(key_list[11], (RANK, D), ((0, 4), (1, 8)), -0.2, 0.2)), 0.003, 0.05)
    mean_output = draw_mean_output(jax.random.fold_in(key_list[14], 71), 0)
    var_output = jnp.clip(jnp.exp(math.log(0.05) - 2.8134107 * jax.random.uniform(key_list[13], (RANK, D), jnp.float32) ** steps_of(key_list[13], (RANK, D), ((0, 4), (1, 8)), -0.2, 0.2)), 0.003, 0.05)
    return dict(hidden_in=hidden_in, forget_pre=forget_pre, forget_cot=forget_cot, lower_bound=lower_bound, head_out=head_out, out_cot=out_cot, basis_forget=basis_forget, basis_output=basis_output, weight_forget=weight_forget, weight_output=weight_output, mean_forget=mean_forget, var_forget=var_forget, mean_output=mean_output, var_output=var_output)


beta_one = 0.9
beta_two = 0.99
adam_eps = 1e-08
norm_eps = 1e-06
step_rate = 0.02

def moment_update(mean, var, proj):
    mean_new = beta_one * mean + (1.0 - beta_one) * proj
    var_new = beta_two * var + (1.0 - beta_two) * proj * proj
    return (mean_new, var_new, mean_new / (jnp.sqrt(var_new) + adam_eps))

def reference(hidden_in, forget_pre, forget_cot, lower_bound, head_out, out_cot, basis_forget, basis_output, weight_forget, weight_output, mean_forget, var_forget, mean_output, var_output):
    sigmoid_z = jax.nn.sigmoid(forget_pre.astype(jnp.float32))
    keep_rate = 1.0 - lower_bound
    forget_val = lower_bound + keep_rate * sigmoid_z
    gate_grad = (forget_cot.astype(jnp.float32) * keep_rate * sigmoid_z * (1.0 - sigmoid_z) / forget_val).astype(jnp.bfloat16)
    grad_forget = jnp.dot(gate_grad.T, hidden_in, preferred_element_type=jnp.float32)
    grad_output = jnp.dot(head_out.T, out_cot, preferred_element_type=jnp.float32)
    highest = lax.Precision.HIGHEST
    basis_f = basis_forget.astype(jnp.float32)
    basis_o = basis_output.astype(jnp.float32)
    proj_forget = jnp.dot(basis_f.T, grad_forget, precision=highest)
    proj_output = jnp.dot(basis_o.T, grad_output, precision=highest)
    mean_f, var_f, dir_forget = moment_update(mean_forget, var_forget, proj_forget)
    mean_o, var_o, dir_output = moment_update(mean_output, var_output, proj_output)
    upd_forget = jnp.dot(basis_f, dir_forget, precision=highest)
    upd_output = jnp.dot(basis_o, dir_output, precision=highest)
    step_forget = upd_forget * lax.rsqrt(jnp.mean(upd_forget * upd_forget) + norm_eps)
    step_output = (upd_output * lax.rsqrt(jnp.mean(upd_output * upd_output) + norm_eps)).T
    new_forget = weight_forget - step_rate * step_forget
    new_output = weight_output - step_rate * step_output
    return (step_forget, step_output, new_forget, new_output, mean_f, var_f, mean_o, var_o, new_forget.astype(jnp.bfloat16), new_output.astype(jnp.bfloat16))
```

```python
import functools

import jax
import jax.numpy as jnp
from jax import lax
from jax.experimental import pallas as pl
from jax.experimental.pallas import tpu as pltpu
from jax.sharding import PartitionSpec as P

MESH = pl.DeviceIdType.MESH
LANES = 128
SUBLANES = 8
CORES = 2

beta_one = 0.9
beta_two = 0.99
adam_eps = 1e-08
norm_eps = 1e-06
step_rate = 0.02


def moment_update(mean, var, proj):
    mean_new = beta_one * mean + (1.0 - beta_one) * proj
    var_new = beta_two * var + (1.0 - beta_two) * proj * proj
    return (mean_new, var_new, mean_new / (jnp.sqrt(var_new) + adam_eps))


def comm_kernel(
    n_fs,
    n_tp,
    total,
    ho_h, fp_h, fc_h, lb_ref, bo_h, bf_h, wo_h, wf_h, oc_h, hi_h, mo_h, vo_h, mf_h, vf_h,
    dir_ref, proj_ref, scale_ref, wall_o, wall_f,
    ho, fp, fc, bo, bf, wo, wf, oc, hi, mo, vo, mf, vf,
    own, psnd, prcv, zsnd, zrcv, coords, gsnd, grcv, pown, wsnd, ssnd, srcv, gram,
    ld, pair_s, pair_r, z_s, z_r, ag_s, ag_r, pp_s, pp_r, g_s, g_r, d_s, d_r, w_s, w_r, wl, s_s, s_r,
):
    n_z = n_tp // CORES
    fs = lax.axis_index("fs")
    tp = lax.axis_index("tp")
    z = tp // CORES
    core = lax.rem(tp, CORES)
    partner = z * CORES + (1 - core)
    tokens, units = ho.shape
    rank = bo.shape[1]
    half = tokens // CORES
    quarter = half // n_z
    part = rank // n_fs

    def z_peer(d):
        return lax.rem(z + d, n_z) * CORES + core

    def fs_peer(d):
        return lax.rem(fs + d, n_fs)

    def remote(src, dst, ssem, rsem, **where):
        return pltpu.make_async_remote_copy(
            src_ref=src, dst_ref=dst, send_sem=ssem, recv_sem=rsem,
            device_id=where, device_id_type=MESH,
        )

    loads = [
        pltpu.make_async_copy(s, d, ld.at[i])
        for i, (s, d) in enumerate((
            (ho_h, ho), (bo_h, bo), (wo_h, wo), (wf_h, wf), (fp_h, fp), (fc_h, fc), (bf_h, bf),
            (oc_h, oc), (hi_h, hi), (mo_h, mo), (vo_h, vo), (mf_h, mf), (vf_h, vf),
        ))
    ]
    (l_ho, l_bo, l_wo, l_wf, l_fp, l_fc, l_bf, l_oc, l_hi, l_mo, l_vo, l_mf, l_vf) = loads
    for l in loads:
        l.start()

    barrier = pltpu.get_barrier_semaphore()
    for d in range(1, n_tp):
        pl.semaphore_signal(barrier, inc=1, device_id={"tp": lax.rem(tp + d, n_tp)}, device_id_type=MESH)
    for d in range(1, n_fs):
        pl.semaphore_signal(barrier, inc=1, device_id={"fs": fs_peer(d)}, device_id_type=MESH)

    l_wo.wait()
    wsnd[0] = wo[...].astype(jnp.bfloat16)
    l_wf.wait()
    wsnd[1] = wf[...].astype(jnp.bfloat16)

    def rows_at(which, i):
        return pl.ds(pl.multiple_of(which * half + i * quarter, quarter), quarter)

    def local_rows(b):
        return b[pl.ds(pl.multiple_of(tp * units, units), units), :]

    l_ho.wait()
    l_bo.wait()

    def coord_o(which, i):
        return jnp.dot(ho[rows_at(which, i), :], local_rows(bo), preferred_element_type=jnp.float32)

    l_fp.wait()
    l_fc.wait()
    l_bf.wait()

    def coord_f(which, i):
        rows = rows_at(which, i)
        e = jnp.exp(-fp[rows, :].astype(jnp.float32))
        lb = lb_ref[...]
        gate = fc[rows, :].astype(jnp.float32) * (1.0 - lb) * e / ((1.0 + e) * (1.0 + lb * e))
        return jnp.dot(gate.astype(jnp.bfloat16), local_rows(bf), preferred_element_type=jnp.float32)

    coord = (coord_o, coord_f)
    pair = [remote(psnd.at[m], prcv.at[m], pair_s.at[m], pair_r.at[m], tp=partner) for m in range(2)]

    def away(m):
        def body(i, carry):
            psnd[m, pl.ds(pl.multiple_of(i * quarter, quarter), quarter), :] = coord[m](1 - core, i).astype(
                jnp.bfloat16
            )
            return carry

        lax.fori_loop(0, n_z, body, 0)

    def home(m):
        def body(i, carry):
            own[m, pl.ds(pl.multiple_of(i * quarter, quarter), quarter), :] = coord[m](core, i)
            return carry

        lax.fori_loop(0, n_z, body, 0)

    away(0)
    pl.semaphore_wait(barrier, n_tp - 1 + n_fs - 1)
    weights = []
    for m, wall in ((0, wall_o), (1, wall_f)):
        for d in range(1, n_fs):
            c = remote(wsnd.at[m], wall.at[fs], w_s.at[m, d], w_r.at[m, d], fs=fs_peer(d))
            weights.append(c)
            c.start()
        c = pltpu.make_async_copy(wsnd.at[m], wall.at[fs], wl.at[m])
        c.start()
        weights.append(c)
    pair[0].start()
    away(1)
    pair[1].start()
    home(0)

    def chunk(ref, m, j):
        return ref.at[m, pl.ds(pl.multiple_of(j * quarter, quarter), quarter)]

    order = sorted(range(1, n_z), key=lambda d: abs(d - n_z // 2))

    def scatter(m):
        pair[m].wait_recv()

        def body(i, carry):
            rows = pl.ds(pl.multiple_of(i * quarter, quarter), quarter)
            added = own[m, rows, :] + prcv[m, rows, :].astype(jnp.float32)
            own[m, rows, :] = added
            zsnd[m, rows, :] = added.astype(jnp.bfloat16)
            return carry

        lax.fori_loop(0, n_z, body, 0)
        sends = []
        for d in order:
            c = remote(
                chunk(zsnd, m, lax.rem(z + d, n_z)), zrcv.at[m, d], z_s.at[m, d], z_r.at[m, d], tp=z_peer(d)
            )
            c.start()
            sends.append(c)
        return sends

    scat = [scatter(0)]
    home(1)
    scat.append(scatter(1))

    for m, b in ((0, bo), (1, bf)):
        g = lax.dot_general(b[...], b[...], (((0,), (0,)), ((), ())), preferred_element_type=jnp.float32)
        upper = g.astype(jnp.bfloat16)
        gram[m, 0] = upper
        gram[m, 1] = (g - upper.astype(jnp.float32)).astype(jnp.bfloat16)

    def spot(which, j):
        return pl.ds(pl.multiple_of(which * half + j * quarter, quarter), quarter)

    def forward(m, d):
        rows = coords.at[m, spot(core, lax.rem(z + n_z - d, n_z))]
        return remote(rows, rows, pp_s.at[m, d], pp_r.at[m, d], tp=partner)

    def gather(m):
        for c in scat[m]:
            c.wait_recv()
        sums = own[m, pl.ds(pl.multiple_of(z * quarter, quarter), quarter), :]
        for d in range(1, n_z):
            sums = sums + zrcv[m, d].astype(jnp.float32)
        coords[m, spot(core, z), :] = sums.astype(jnp.bfloat16)
        rows = coords.at[m, spot(core, z)]
        sends = []
        for d in order:
            c = remote(rows, rows, ag_s.at[m, d], ag_r.at[m, d], tp=z_peer(d))
            c.start()
            sends.append((d, c))
        f = forward(m, 0)
        f.start()
        return sends, [f]

    gat = [gather(0), gather(1)]

    data = ((oc, l_oc), (hi, l_hi))

    def project(m):
        sends, fwd = gat[m]
        for d, c in sends:
            c.wait_recv()
            f = forward(m, d)
            f.start()
            fwd.append(f)
        data[m][1].wait()
        for f in fwd:
            f.wait_recv()
        proj = lax.dot_general(
            coords[m], data[m][0][...], (((0,), (0,)), ((), ())), preferred_element_type=jnp.float32
        )
        pown[m] = proj
        gsnd[m] = proj.astype(jnp.bfloat16)
        out = []
        for d in range(1, n_fs):
            c = remote(
                gsnd.at[m, pl.ds(pl.multiple_of(fs_peer(d) * part, part), part)],
                grcv.at[m, d], g_s.at[m, d], g_r.at[m, d], fs=fs_peer(d),
            )
            c.start()
            out.append(c)
        return out

    red = [project(0), project(1)]
    moments = (((mo, l_mo), (vo, l_vo)), ((mf, l_mf), (vf, l_vf)))
    own_ranks = pl.ds(pl.multiple_of(fs * part, part), part)

    def direct(m):
        for c in red[m]:
            c.wait_recv()
        proj = pown[m, own_ranks, :]
        for d in range(1, n_fs):
            proj = proj + grcv[m, d].astype(jnp.float32)
        proj_ref[m] = proj
        for _, l in moments[m]:
            l.wait()
        direction = moment_update(moments[m][0][0][...], moments[m][1][0][...], proj)[2]
        dir_ref[m, own_ranks, :] = direction.astype(jnp.bfloat16)
        mine = dir_ref.at[m, own_ranks]
        out = []
        for d in range(1, n_fs):
            c = remote(mine, mine, d_s.at[m, d], d_r.at[m, d], fs=fs_peer(d))
            c.start()
            out.append(c)
        return out

    spread = [direct(0), direct(1)]
    squares = []
    for m in range(2):
        for c in spread[m]:
            c.wait_recv()
        v = dir_ref[m]
        gv = jnp.dot(gram[m, 0], v, preferred_element_type=jnp.float32)
        gv = gv + jnp.dot(gram[m, 1], v, preferred_element_type=jnp.float32)
        squares.append(jnp.sum(v.astype(jnp.float32) * gv))
    row = lax.broadcasted_iota(jnp.int32, ssnd.shape, 0)
    mine = jnp.where(row < SUBLANES // 2, squares[0], squares[1])
    ssnd[...] = mine
    tells = []
    for d in range(1, n_tp):
        c = remote(ssnd, srcv.at[d], s_s.at[d], s_r.at[d], tp=lax.rem(tp + d, n_tp))
        c.start()
        tells.append(c)
    srcv[0] = mine
    for c in tells:
        c.wait_recv()
    acc = jnp.zeros(ssnd.shape, jnp.float32)
    for t in range(n_tp):
        acc = acc + srcv[lax.rem(tp + n_tp - t, n_tp)]
    scale_ref[...] = lax.rsqrt(acc / total + norm_eps)

    for c in weights:
        c.wait()
    for m in range(2):
        pair[m].wait_send()
        for c in scat[m] + [c for _, c in gat[m][0]] + gat[m][1] + red[m] + spread[m]:
            c.wait_send()
    for c in tells:
        c.wait_send()


def finish_kernel(
    scale_ref, dir_ref, bo_ref, bf_ref, wall_o, wall_f, wo_ref, wf_ref, proj_ref, mo, vo, mf, vf,
    step_f, step_o, new_f, new_o, mf_n, vf_n, mo_n, vo_n, copy_f, copy_o, dir_t,
):
    k = pl.program_id(0)
    fs = lax.axis_index("fs")

    @pl.when(k == 0)
    def _():
        dir_t[...] = dir_ref[0].astype(jnp.float32).T.astype(jnp.bfloat16)
        mean, var, _ = moment_update(mo[...], vo[...], proj_ref[0])
        mo_n[...] = mean
        vo_n[...] = var
        mean, var, _ = moment_update(mf[...], vf[...], proj_ref[1])
        mf_n[...] = mean
        vf_n[...] = var

    scale_o = scale_ref[0:1, 0:1]
    scale_f = scale_ref[SUBLANES // 2 : SUBLANES // 2 + 1, 0:1]
    upd_f = jnp.dot(bf_ref[...], dir_ref[1], preferred_element_type=jnp.float32) * scale_f
    copy_f[...] = (wall_f[0].astype(jnp.float32) - step_rate * upd_f).astype(jnp.bfloat16)
    upd_o = (
        lax.dot_general(
            dir_t[...], bo_ref[...], (((1,), (1,)), ((), ())), preferred_element_type=jnp.float32
        )
        * scale_o
    )
    copy_o[...] = (wall_o[0].astype(jnp.float32) - step_rate * upd_o).astype(jnp.bfloat16)

    @pl.when(k == fs)
    def _():
        step_f[...] = upd_f
        new_f[...] = wf_ref[...] - step_rate * upd_f
        step_o[...] = upd_o
        new_o[...] = wo_ref[...] - step_rate * upd_o


def kernels_device(
    n_fs, n_tp, hidden_in, forget_pre, forget_cot, lower_bound, head_out, out_cot, basis_forget, basis_output,
    weight_forget, weight_output, mean_forget, var_forget, mean_output, var_output,
):
    tokens, units = head_out.shape
    feats = hidden_in.shape[1]
    rows = weight_forget.shape[0]
    channels, rank = basis_forget.shape
    part = rank // n_fs
    n_z = n_tp // CORES
    half = tokens // CORES
    quarter = half // n_z
    bf16, f32 = jnp.bfloat16, jnp.float32
    shape = jax.ShapeDtypeStruct
    anywhere = pl.BlockSpec(memory_space=pl.ANY)
    vmem = pl.BlockSpec(memory_space=pltpu.VMEM)
    dma = pltpu.SemaphoreType.DMA
    inputs = (
        head_out, forget_pre, forget_cot, lower_bound.reshape(1, units), basis_output, basis_forget,
        weight_output, weight_forget, out_cot, hidden_in, mean_output, var_output, mean_forget, var_forget,
    )
    directions, proj, scale, wall_o, wall_f = pl.pallas_call(
        functools.partial(comm_kernel, n_fs, n_tp, float(channels * feats * n_tp)),
        out_shape=(
            shape((2, rank, feats), bf16),
            shape((2, part, feats), f32),
            shape((SUBLANES, LANES), f32),
            shape((n_fs,) + weight_output.shape, bf16),
            shape((n_fs,) + weight_forget.shape, bf16),
        ),
        in_specs=[anywhere] * 3 + [vmem] + [anywhere] * 10,
        out_specs=(vmem, vmem, vmem, anywhere, anywhere),
        scratch_shapes=[
            pltpu.VMEM(a.shape, a.dtype)
            for a in (
                head_out, forget_pre, forget_cot, basis_output, basis_forget, weight_output, weight_forget,
                out_cot, hidden_in, mean_output, var_output, mean_forget, var_forget,
            )
        ]
        + [
            pltpu.VMEM((2, half, rank), f32),
            pltpu.VMEM((2, half, rank), bf16),
            pltpu.VMEM((2, half, rank), bf16),
            pltpu.VMEM((2, half, rank), bf16),
            pltpu.VMEM((2, n_z, quarter, rank), bf16),
            pltpu.VMEM((2, tokens, rank), bf16),
            pltpu.VMEM((2, rank, feats), bf16),
            pltpu.VMEM((2, n_fs, part, feats), bf16),
            pltpu.VMEM((2, rank, feats), f32),
            pltpu.VMEM((2,) + weight_forget.shape, bf16),
            pltpu.VMEM((SUBLANES, LANES), f32),
            pltpu.VMEM((n_tp, SUBLANES, LANES), f32),
            pltpu.VMEM((2, 2, rank, rank), bf16),
            dma((13,)),
            dma((2,)), dma((2,)),
            dma((2, n_z)), dma((2, n_z)), dma((2, n_z)), dma((2, n_z)), dma((2, n_z)), dma((2, n_z)),
            dma((2, n_fs)), dma((2, n_fs)), dma((2, n_fs)), dma((2, n_fs)), dma((2, n_fs)), dma((2, n_fs)),
            dma((2,)),
            dma((n_tp,)), dma((n_tp,)),
        ],
        compiler_params=pltpu.CompilerParams(
            collective_id=0, has_side_effects=True, vmem_limit_bytes=60 * 2**20
        ),
    )(*inputs)

    def whole(a):
        return pl.BlockSpec(a.shape, lambda k, n=len(a.shape): (0,) * n)

    def outs(a):
        return whole(shape(a.shape, f32))

    outputs = pl.pallas_call(
        finish_kernel,
        grid=(n_fs,),
        out_shape=tuple(
            shape(a.shape, f32)
            for a in (
                weight_forget, weight_output, weight_forget, weight_output, mean_forget, var_forget,
                mean_output, var_output,
            )
        )
        + (shape((channels, feats), bf16), shape((feats, channels), bf16)),
        in_specs=[
            whole(scale),
            whole(directions),
            pl.BlockSpec((rows, rank), lambda k: (k, 0)),
            pl.BlockSpec((rows, rank), lambda k: (k, 0)),
            pl.BlockSpec((1,) + weight_output.shape, lambda k: (k, 0, 0)),
            pl.BlockSpec((1,) + weight_forget.shape, lambda k: (k, 0, 0)),
            whole(weight_output),
            whole(weight_forget),
            whole(proj),
            whole(mean_output),
            whole(var_output),
            whole(mean_forget),
            whole(var_forget),
        ],
        out_specs=tuple(
            outs(a)
            for a in (
                weight_forget, weight_output, weight_forget, weight_output, mean_forget, var_forget,
                mean_output, var_output,
            )
        )
        + (
            pl.BlockSpec((rows, feats), lambda k: (k, 0)),
            pl.BlockSpec((feats, rows), lambda k: (0, k)),
        ),
        scratch_shapes=[pltpu.VMEM((feats, rank), bf16)],
        compiler_params=pltpu.CompilerParams(
            dimension_semantics=("arbitrary",), vmem_limit_bytes=48 * 2**20
        ),
    )(
        scale, directions, basis_output, basis_forget, wall_o, wall_f, weight_output, weight_forget, proj,
        mean_output, var_output, mean_forget, var_forget,
    )
    return outputs


def split_product(coords, tokens_data):
    upper = coords.astype(jnp.bfloat16)
    lower = (coords - upper.astype(jnp.float32)).astype(jnp.bfloat16)
    first = jnp.einsum("tr,td->rd", upper, tokens_data, preferred_element_type=jnp.float32)
    second = jnp.einsum("tr,td->rd", lower, tokens_data, preferred_element_type=jnp.float32)
    return first + second


def per_device(
    hidden_in,
    forget_pre,
    forget_cot,
    lower_bound,
    head_out,
    out_cot,
    basis_forget,
    basis_output,
    weight_forget,
    weight_output,
    mean_forget,
    var_forget,
    mean_output,
    var_output,
):
    highest = lax.Precision.HIGHEST
    fs_rank = lax.axis_index("fs")
    tp_rank = lax.axis_index("tp")
    unit_count = forget_pre.shape[1]
    feat_cols = hidden_in.shape[1]
    head_rows = weight_forget.shape[0]
    sigmoid_z = jax.nn.sigmoid(forget_pre.astype(jnp.float32))
    keep_rate = 1.0 - lower_bound
    forget_val = lower_bound + keep_rate * sigmoid_z
    gate_grad = (
        forget_cot.astype(jnp.float32) * keep_rate * sigmoid_z * (1.0 - sigmoid_z) / forget_val
    ).astype(jnp.bfloat16)
    rows_forget = lax.dynamic_slice_in_dim(basis_forget, fs_rank * head_rows, head_rows, 0).astype(
        jnp.float32
    )
    rows_output = lax.dynamic_slice_in_dim(basis_output, fs_rank * head_rows, head_rows, 0).astype(
        jnp.float32
    )
    local_forget = lax.dynamic_slice_in_dim(basis_forget, tp_rank * unit_count, unit_count, 0)
    local_output = lax.dynamic_slice_in_dim(basis_output, tp_rank * unit_count, unit_count, 0)
    coords_forget = jnp.dot(gate_grad, local_forget, preferred_element_type=jnp.float32)
    coords_output = jnp.dot(head_out, local_output, preferred_element_type=jnp.float32)
    coords_forget, coords_output = lax.psum((coords_forget, coords_output), "tp")
    part_forget = split_product(coords_forget, hidden_in)
    part_output = split_product(coords_output, out_cot)
    proj = lax.psum_scatter(
        jnp.concatenate([part_forget, part_output], axis=1), "fs", scatter_dimension=0, tiled=True
    )
    mean_f, var_f, dir_forget = moment_update(mean_forget, var_forget, proj[:, :feat_cols])
    mean_o, var_o, dir_output = moment_update(mean_output, var_output, proj[:, feat_cols:])
    dir_forget, dir_output = (
        lax.all_gather(dir_forget, "fs", axis=0, tiled=True),
        lax.all_gather(dir_output, "fs", axis=0, tiled=True),
    )
    upd_forget = jnp.dot(rows_forget, dir_forget, precision=highest)
    upd_output = jnp.dot(rows_output, dir_output, precision=highest)
    total = float(basis_forget.shape[0] * feat_cols * lax.axis_size("tp"))
    sum_forget, sum_output = lax.psum(
        (jnp.sum(upd_forget * upd_forget), jnp.sum(upd_output * upd_output)), ("fs", "tp")
    )
    step_forget = upd_forget * lax.rsqrt(sum_forget / total + norm_eps)
    step_output = (upd_output * lax.rsqrt(sum_output / total + norm_eps)).T
    new_forget = weight_forget - step_rate * step_forget
    new_output = weight_output - step_rate * step_output
    copy_forget, copy_output = (
        lax.all_gather(new_forget.astype(jnp.bfloat16), "fs", axis=0, tiled=True),
        lax.all_gather(new_output.astype(jnp.bfloat16), "fs", axis=1, tiled=True),
    )
    return (
        step_forget,
        step_output,
        new_forget,
        new_output,
        mean_f,
        var_f,
        mean_o,
        var_o,
        copy_forget,
        copy_output,
    )


def fits(n_fs, n_tp, forget_pre, hidden_in, basis):
    tokens, units = forget_pre.shape
    quarter = tokens // n_tp
    part = basis.shape[1] // n_fs
    return (
        n_tp % CORES == 0
        and n_tp > CORES
        and n_fs > 1
        and tokens % n_tp == 0
        and units % LANES == 0
        and hidden_in.shape[1] % LANES == 0
        and quarter % (2 * SUBLANES) == 0
        and part % (2 * SUBLANES) == 0
    )


def device_step(n_fs, n_tp, *args):
    if fits(n_fs, n_tp, args[1], args[0], args[6]):
        return kernels_device(n_fs, n_tp, *args)
    return per_device(*args)


def solution(mesh):
    return jax.shard_map(
        functools.partial(device_step, mesh.shape["fs"], mesh.shape["tp"]),
        mesh=mesh,
        in_specs=(
            P("fs", "tp"),
            P("fs", "tp"),
            P("fs", "tp"),
            P("tp"),
            P("fs", "tp"),
            P("fs", "tp"),
            P(),
            P(),
            P("fs", "tp"),
            P("tp", "fs"),
            P("fs", "tp"),
            P("fs", "tp"),
            P("fs", "tp"),
            P("fs", "tp"),
        ),
        out_specs=(
            P("fs", "tp"),
            P("tp", "fs"),
            P("fs", "tp"),
            P("tp", "fs"),
            P("fs", "tp"),
            P("fs", "tp"),
            P("fs", "tp"),
            P("fs", "tp"),
            P(None, "tp"),
            P("tp", None),
        ),
        check_vma=False,
    )
```

```python
import functools

import jax
import jax.numpy as jnp
from jax import lax
from jax.experimental import pallas as pl
from jax.experimental.pallas import tpu as pltpu
from jax.sharding import PartitionSpec as P

MESH = pl.DeviceIdType.MESH
LANES = 128
SUBLANES = 8
CORES = 2

beta_one = 0.9
beta_two = 0.99
adam_eps = 1e-08
norm_eps = 1e-06
step_rate = 0.02


def moment_update(mean, var, proj):
    mean_new = beta_one * mean + (1.0 - beta_one) * proj
    var_new = beta_two * var + (1.0 - beta_two) * proj * proj
    return (mean_new, var_new, mean_new / (jnp.sqrt(var_new) + adam_eps))


def comm_kernel(
    n_fs,
    n_tp,
    total,
    ho_h, fp_h, fc_h, lb_ref, bo_h, bf_h, wo_h, wf_h, oc_h, hi_h, mo_h, vo_h, mf_h, vf_h,
    dir_ref, proj_ref, scale_ref, wall_o, wall_f,
    ho, fp, fc, bo, bf, wo, wf, oc, hi, mo, vo, mf, vf,
    own, psnd, prcv, zsnd, zrcv, coords, gsnd, grcv, pown, wsnd, ssnd, srcv, gram,
    ld, pair_s, pair_r, z_s, z_r, ag_s, ag_r, pp_s, pp_r, g_s, g_r, d_s, d_r, w_s, w_r, wl, s_s, s_r,
):
    n_z = n_tp // CORES
    fs = lax.axis_index("fs")
    tp = lax.axis_index("tp")
    z = tp // CORES
    core = lax.rem(tp, CORES)
    partner = z * CORES + (1 - core)
    tokens, units = ho.shape
    rank = bo.shape[1]
    half = tokens // CORES
    quarter = half // n_z
    part = rank // n_fs

    def z_peer(d):
        return lax.rem(z + d, n_z) * CORES + core

    def fs_peer(d):
        return lax.rem(fs + d, n_fs)

    def remote(src, dst, ssem, rsem, **where):
        return pltpu.make_async_remote_copy(
            src_ref=src, dst_ref=dst, send_sem=ssem, recv_sem=rsem,
            device_id=where, device_id_type=MESH,
        )

    loads = [
        pltpu.make_async_copy(s, d, ld.at[i])
        for i, (s, d) in enumerate((
            (ho_h, ho), (bo_h, bo), (fp_h, fp), (fc_h, fc), (bf_h, bf), (wo_h, wo), (wf_h, wf),
            (oc_h, oc), (hi_h, hi), (mo_h, mo), (vo_h, vo), (mf_h, mf), (vf_h, vf),
        ))
    ]
    (l_ho, l_bo, l_fp, l_fc, l_bf, l_wo, l_wf, l_oc, l_hi, l_mo, l_vo, l_mf, l_vf) = loads
    for l in loads:
        l.start()

    barrier = pltpu.get_barrier_semaphore()
    for d in range(1, n_tp):
        pl.semaphore_signal(barrier, inc=1, device_id={"tp": lax.rem(tp + d, n_tp)}, device_id_type=MESH)
    for d in range(1, n_fs):
        pl.semaphore_signal(barrier, inc=1, device_id={"fs": fs_peer(d)}, device_id_type=MESH)

    def rows_at(which, i):
        return pl.ds(pl.multiple_of(which * half + i * quarter, quarter), quarter)

    def local_rows(b):
        return b[pl.ds(pl.multiple_of(tp * units, units), units), :]

    l_ho.wait()
    l_bo.wait()

    def coord_o(which, i):
        return jnp.dot(ho[rows_at(which, i), :], local_rows(bo), preferred_element_type=jnp.float32)

    def coord_f(which, i):
        rows = rows_at(which, i)
        e = jnp.exp(-fp[rows, :].astype(jnp.float32))
        lb = lb_ref[...]
        gate = fc[rows, :].astype(jnp.float32) * (1.0 - lb) * e / ((1.0 + e) * (1.0 + lb * e))
        return jnp.dot(gate.astype(jnp.bfloat16), local_rows(bf), preferred_element_type=jnp.float32)

    coord = (coord_o, coord_f)
    pair = [remote(psnd.at[m], prcv.at[m], pair_s.at[m], pair_r.at[m], tp=partner) for m in range(2)]

    def away(m):
        def body(i, carry):
            psnd[m, pl.ds(pl.multiple_of(i * quarter, quarter), quarter), :] = coord[m](1 - core, i).astype(
                jnp.bfloat16
            )
            return carry

        lax.fori_loop(0, n_z, body, 0)

    def home(m):
        def body(i, carry):
            own[m, pl.ds(pl.multiple_of(i * quarter, quarter), quarter), :] = coord[m](core, i)
            return carry

        lax.fori_loop(0, n_z, body, 0)

    away(0)
    pl.semaphore_wait(barrier, n_tp - 1 + n_fs - 1)
    pair[0].start()

    x, y = lax.rem(fs, 2), fs // 2
    beside, above = y * 2 + 1 - x, (1 - y) * 2 + x
    walls = (wall_o, wall_f)

    def send_weights(m):
        wall = walls[m]
        load, source = ((l_wo, wo), (l_wf, wf))[m]
        load.wait()
        wsnd[m] = source[...].astype(jnp.bfloat16)
        sent = []
        if n_fs == 4:
            peers = (beside, above)
        else:
            peers = [fs_peer(d) for d in range(1, n_fs)]
        for i, peer in enumerate(peers):
            c = remote(wsnd.at[m], wall.at[fs], w_s.at[m, i], w_r.at[m, i], fs=peer)
            c.start()
            sent.append(c)
        kept = pltpu.make_async_copy(wsnd.at[m], wall.at[fs], wl.at[m])
        kept.start()
        return sent, kept

    def relay_weights(m):
        if n_fs != 4:
            return []
        sent = weights[m][0]
        rows = walls[m].shape[1] // 2
        passed = []
        for i, (origin, target) in enumerate(((beside, above), (above, beside))):
            sent[i].wait_recv()
            piece = walls[m].at[origin, pl.ds(i * rows, rows)]
            c = remote(piece, piece, w_s.at[m, 2 + i], w_r.at[m, 2 + i], fs=target)
            c.start()
            passed.append(c)
        return passed

    weights = [send_weights(0)]
    l_fp.wait()
    l_fc.wait()
    l_bf.wait()
    away(1)
    pair[1].start()
    weights.append(send_weights(1))
    home(0)

    def chunk(ref, m, j):
        return ref.at[m, pl.ds(pl.multiple_of(j * quarter, quarter), quarter)]

    order = sorted(range(1, n_z), key=lambda d: abs(d - n_z // 2))

    def scatter(m):
        pair[m].wait_recv()

        def body(i, carry):
            rows = pl.ds(pl.multiple_of(i * quarter, quarter), quarter)
            added = own[m, rows, :] + prcv[m, rows, :].astype(jnp.float32)
            own[m, rows, :] = added
            zsnd[m, rows, :] = added.astype(jnp.bfloat16)
            return carry

        lax.fori_loop(0, n_z, body, 0)
        sends = []
        for d in order:
            c = remote(
                chunk(zsnd, m, lax.rem(z + d, n_z)), zrcv.at[m, d], z_s.at[m, d], z_r.at[m, d], tp=z_peer(d)
            )
            c.start()
            sends.append(c)
        return sends

    scat = [scatter(0)]
    home(1)
    scat.append(scatter(1))

    for m, b in ((0, bo), (1, bf)):
        g = lax.dot_general(b[...], b[...], (((0,), (0,)), ((), ())), preferred_element_type=jnp.float32)
        upper = g.astype(jnp.bfloat16)
        gram[m, 0] = upper
        gram[m, 1] = (g - upper.astype(jnp.float32)).astype(jnp.bfloat16)

    def spot(which, j):
        return pl.ds(pl.multiple_of(which * half + j * quarter, quarter), quarter)

    def forward(m, d):
        rows = coords.at[m, spot(core, lax.rem(z + n_z - d, n_z))]
        return remote(rows, rows, pp_s.at[m, d], pp_r.at[m, d], tp=partner)

    def gather(m):
        for c in scat[m]:
            c.wait_recv()
        sums = own[m, pl.ds(pl.multiple_of(z * quarter, quarter), quarter), :]
        for d in range(1, n_z):
            sums = sums + zrcv[m, d].astype(jnp.float32)
        coords[m, spot(core, z), :] = sums.astype(jnp.bfloat16)
        rows = coords.at[m, spot(core, z)]
        sends = []
        for d in order:
            c = remote(rows, rows, ag_s.at[m, d], ag_r.at[m, d], tp=z_peer(d))
            c.start()
            sends.append((d, c))
        f = forward(m, 0)
        f.start()
        return sends, [f]

    gat = [gather(0)]
    passed = [relay_weights(0)]
    gat.append(gather(1))
    passed.append(relay_weights(1))

    data = ((oc, l_oc), (hi, l_hi))

    def project(m):
        sends, fwd = gat[m]
        for d, c in sends:
            c.wait_recv()
            f = forward(m, d)
            f.start()
            fwd.append(f)
        data[m][1].wait()
        for f in fwd:
            f.wait_recv()
        proj = lax.dot_general(
            coords[m], data[m][0][...], (((0,), (0,)), ((), ())), preferred_element_type=jnp.float32
        )
        pown[m] = proj
        gsnd[m] = proj.astype(jnp.bfloat16)
        out = []
        for d in range(1, n_fs):
            c = remote(
                gsnd.at[m, pl.ds(pl.multiple_of(fs_peer(d) * part, part), part)],
                grcv.at[m, d], g_s.at[m, d], g_r.at[m, d], fs=fs_peer(d),
            )
            c.start()
            out.append(c)
        return out

    red = [project(0), project(1)]
    moments = (((mo, l_mo), (vo, l_vo)), ((mf, l_mf), (vf, l_vf)))
    own_ranks = pl.ds(pl.multiple_of(fs * part, part), part)

    def direct(m):
        for c in red[m]:
            c.wait_recv()
        proj = pown[m, own_ranks, :]
        for d in range(1, n_fs):
            proj = proj + grcv[m, d].astype(jnp.float32)
        proj_ref[m] = proj
        for _, l in moments[m]:
            l.wait()
        direction = moment_update(moments[m][0][0][...], moments[m][1][0][...], proj)[2]
        dir_ref[m, own_ranks, :] = direction.astype(jnp.bfloat16)
        mine = dir_ref.at[m, own_ranks]
        out = []
        for d in range(1, n_fs):
            c = remote(mine, mine, d_s.at[m, d], d_r.at[m, d], fs=fs_peer(d))
            c.start()
            out.append(c)
        return out

    spread = [direct(0), direct(1)]
    squares = []
    for m in range(2):
        for c in spread[m]:
            c.wait_recv()
        v = dir_ref[m]
        gv = jnp.dot(gram[m, 0], v, preferred_element_type=jnp.float32)
        gv = gv + jnp.dot(gram[m, 1], v, preferred_element_type=jnp.float32)
        squares.append(jnp.sum(v.astype(jnp.float32) * gv))
    row = lax.broadcasted_iota(jnp.int32, ssnd.shape, 0)
    mine = jnp.where(row < SUBLANES // 2, squares[0], squares[1])
    ssnd[...] = mine
    tells = []
    for d in range(1, n_tp):
        c = remote(ssnd, srcv.at[d], s_s.at[d], s_r.at[d], tp=lax.rem(tp + d, n_tp))
        c.start()
        tells.append(c)
    srcv[0] = mine
    for c in tells:
        c.wait_recv()
    acc = jnp.zeros(ssnd.shape, jnp.float32)
    for t in range(n_tp):
        acc = acc + srcv[lax.rem(tp + n_tp - t, n_tp)]
    scale_ref[...] = lax.rsqrt(acc / total + norm_eps)

    for m in range(2):
        for c in weights[m][0]:
            if n_fs != 4:
                c.wait_recv()
            c.wait_send()
        weights[m][1].wait()
        for c in passed[m]:
            c.wait()
        pair[m].wait_send()
        for c in scat[m] + [c for _, c in gat[m][0]] + gat[m][1] + red[m] + spread[m]:
            c.wait_send()
    for c in tells:
        c.wait_send()


def finish_kernel(
    fs_ref, scale_ref, dir_ref, bo_ref, bf_ref, wall_o, wall_f, wo_h, wf_h, proj_ref, mo, vo, mf, vf,
    step_f_h, step_o_h, new_f_h, new_o_h, mf_n, vf_n, mo_n, vo_n, copy_f, copy_o,
    dir_t, wo, wf, step_f, step_o, new_f, new_o, in_sem, out_sem,
):
    k = pl.program_id(0)
    reads = [pltpu.make_async_copy(s, d, in_sem.at[i]) for i, (s, d) in enumerate(((wo_h, wo), (wf_h, wf)))]
    writes = [
        pltpu.make_async_copy(s, d, out_sem.at[i])
        for i, (s, d) in enumerate(
            ((step_f, step_f_h), (step_o, step_o_h), (new_f, new_f_h), (new_o, new_o_h))
        )
    ]

    @pl.when(k == 0)
    def _():
        for c in reads:
            c.start()
        dir_t[...] = dir_ref[0].astype(jnp.float32).T.astype(jnp.bfloat16)
        mean, var, _ = moment_update(mo[...], vo[...], proj_ref[0])
        mo_n[...] = mean
        vo_n[...] = var
        mean, var, _ = moment_update(mf[...], vf[...], proj_ref[1])
        mf_n[...] = mean
        vf_n[...] = var

    scale_o = scale_ref[0:1, 0:1]
    scale_f = scale_ref[SUBLANES // 2 : SUBLANES // 2 + 1, 0:1]
    upd_f = jnp.dot(bf_ref[...], dir_ref[1], preferred_element_type=jnp.float32) * scale_f
    copy_f[...] = (wall_f[0].astype(jnp.float32) - step_rate * upd_f).astype(jnp.bfloat16)
    upd_o = (
        lax.dot_general(
            dir_t[...], bo_ref[...], (((1,), (1,)), ((), ())), preferred_element_type=jnp.float32
        )
        * scale_o
    )
    copy_o[...] = (wall_o[0].astype(jnp.float32) - step_rate * upd_o).astype(jnp.bfloat16)

    @pl.when(k == 1)
    def _():
        for c in reads:
            c.wait()
        step_f[...] = upd_f
        step_o[...] = upd_o
        new_f[...] = wf[...] - step_rate * upd_f
        new_o[...] = wo[...] - step_rate * upd_o
        for c in writes:
            c.start()

    @pl.when(k == pl.num_programs(0) - 1)
    def _():
        for c in writes:
            c.wait()


def kernels_device(
    n_fs, n_tp, hidden_in, forget_pre, forget_cot, lower_bound, head_out, out_cot, basis_forget, basis_output,
    weight_forget, weight_output, mean_forget, var_forget, mean_output, var_output,
):
    tokens, units = head_out.shape
    feats = hidden_in.shape[1]
    rows = weight_forget.shape[0]
    channels, rank = basis_forget.shape
    part = rank // n_fs
    n_z = n_tp // CORES
    half = tokens // CORES
    quarter = half // n_z
    bf16, f32 = jnp.bfloat16, jnp.float32
    shape = jax.ShapeDtypeStruct
    anywhere = pl.BlockSpec(memory_space=pl.ANY)
    vmem = pl.BlockSpec(memory_space=pltpu.VMEM)
    dma = pltpu.SemaphoreType.DMA
    inputs = (
        head_out, forget_pre, forget_cot, lower_bound.reshape(1, units), basis_output, basis_forget,
        weight_output, weight_forget, out_cot, hidden_in, mean_output, var_output, mean_forget, var_forget,
    )
    directions, proj, scale, wall_o, wall_f = pl.pallas_call(
        functools.partial(comm_kernel, n_fs, n_tp, float(channels * feats * n_tp)),
        out_shape=(
            shape((2, rank, feats), bf16),
            shape((2, part, feats), f32),
            shape((SUBLANES, LANES), f32),
            shape((n_fs,) + weight_output.shape, bf16),
            shape((n_fs,) + weight_forget.shape, bf16),
        ),
        in_specs=[anywhere] * 3 + [vmem] + [anywhere] * 10,
        out_specs=(vmem, vmem, vmem, anywhere, anywhere),
        scratch_shapes=[
            pltpu.VMEM(a.shape, a.dtype)
            for a in (
                head_out, forget_pre, forget_cot, basis_output, basis_forget, weight_output, weight_forget,
                out_cot, hidden_in, mean_output, var_output, mean_forget, var_forget,
            )
        ]
        + [
            pltpu.VMEM((2, half, rank), f32),
            pltpu.VMEM((2, half, rank), bf16),
            pltpu.VMEM((2, half, rank), bf16),
            pltpu.VMEM((2, half, rank), bf16),
            pltpu.VMEM((2, n_z, quarter, rank), bf16),
            pltpu.VMEM((2, tokens, rank), bf16),
            pltpu.VMEM((2, rank, feats), bf16),
            pltpu.VMEM((2, n_fs, part, feats), bf16),
            pltpu.VMEM((2, rank, feats), f32),
            pltpu.VMEM((2,) + weight_forget.shape, bf16),
            pltpu.VMEM((SUBLANES, LANES), f32),
            pltpu.VMEM((n_tp, SUBLANES, LANES), f32),
            pltpu.VMEM((2, 2, rank, rank), bf16),
            dma((13,)),
            dma((2,)), dma((2,)),
            dma((2, n_z)), dma((2, n_z)), dma((2, n_z)), dma((2, n_z)), dma((2, n_z)), dma((2, n_z)),
            dma((2, n_fs)), dma((2, n_fs)), dma((2, n_fs)), dma((2, n_fs)), dma((2, n_fs)), dma((2, n_fs)),
            dma((2,)),
            dma((n_tp,)), dma((n_tp,)),
        ],
        compiler_params=pltpu.CompilerParams(
            collective_id=0, has_side_effects=True, vmem_limit_bytes=60 * 2**20
        ),
    )(*inputs)

    def whole(a):
        return pl.BlockSpec(a.shape, lambda k, r, n=len(a.shape): (0,) * n)

    def turn(k, r):
        return lax.rem(k + r[0] + n_fs - 1, n_fs)

    f32_weights = (weight_forget, weight_output, weight_forget, weight_output)
    f32_moments = (mean_forget, var_forget, mean_output, var_output)
    outputs = pl.pallas_call(
        finish_kernel,
        grid_spec=pltpu.PrefetchScalarGridSpec(
            num_scalar_prefetch=1,
            grid=(n_fs,),
            in_specs=[
                whole(scale),
                whole(directions),
                pl.BlockSpec((rows, rank), lambda k, r: (turn(k, r), 0)),
                pl.BlockSpec((rows, rank), lambda k, r: (turn(k, r), 0)),
                pl.BlockSpec((1,) + weight_output.shape, lambda k, r: (turn(k, r), 0, 0)),
                pl.BlockSpec((1,) + weight_forget.shape, lambda k, r: (turn(k, r), 0, 0)),
                anywhere,
                anywhere,
                whole(proj),
                whole(mean_output),
                whole(var_output),
                whole(mean_forget),
                whole(var_forget),
            ],
            out_specs=[anywhere] * 4
            + [whole(a) for a in f32_moments]
            + [
                pl.BlockSpec((rows, feats), lambda k, r: (turn(k, r), 0)),
                pl.BlockSpec((feats, rows), lambda k, r: (0, turn(k, r))),
            ],
            scratch_shapes=[pltpu.VMEM((feats, rank), bf16)]
            + [pltpu.VMEM(a.shape, f32) for a in (weight_output, weight_forget) + f32_weights]
            + [dma((2,)), dma((4,))],
        ),
        out_shape=tuple(shape(a.shape, f32) for a in f32_weights + f32_moments)
        + (shape((channels, feats), bf16), shape((feats, channels), bf16)),
        compiler_params=pltpu.CompilerParams(
            dimension_semantics=("arbitrary",), vmem_limit_bytes=63 * 2**20
        ),
    )(
        lax.axis_index("fs").reshape(1).astype(jnp.int32),
        scale, directions, basis_output, basis_forget, wall_o, wall_f, weight_output, weight_forget, proj,
        mean_output, var_output, mean_forget, var_forget,
    )
    return outputs


def split_product(coords, tokens_data):
    upper = coords.astype(jnp.bfloat16)
    lower = (coords - upper.astype(jnp.float32)).astype(jnp.bfloat16)
    first = jnp.einsum("tr,td->rd", upper, tokens_data, preferred_element_type=jnp.float32)
    second = jnp.einsum("tr,td->rd", lower, tokens_data, preferred_element_type=jnp.float32)
    return first + second


def per_device(
    hidden_in,
    forget_pre,
    forget_cot,
    lower_bound,
    head_out,
    out_cot,
    basis_forget,
    basis_output,
    weight_forget,
    weight_output,
    mean_forget,
    var_forget,
    mean_output,
    var_output,
):
    highest = lax.Precision.HIGHEST
    fs_rank = lax.axis_index("fs")
    tp_rank = lax.axis_index("tp")
    unit_count = forget_pre.shape[1]
    feat_cols = hidden_in.shape[1]
    head_rows = weight_forget.shape[0]
    sigmoid_z = jax.nn.sigmoid(forget_pre.astype(jnp.float32))
    keep_rate = 1.0 - lower_bound
    forget_val = lower_bound + keep_rate * sigmoid_z
    gate_grad = (
        forget_cot.astype(jnp.float32) * keep_rate * sigmoid_z * (1.0 - sigmoid_z) / forget_val
    ).astype(jnp.bfloat16)
    rows_forget = lax.dynamic_slice_in_dim(basis_forget, fs_rank * head_rows, head_rows, 0).astype(
        jnp.float32
    )
    rows_output = lax.dynamic_slice_in_dim(basis_output, fs_rank * head_rows, head_rows, 0).astype(
        jnp.float32
    )
    local_forget = lax.dynamic_slice_in_dim(basis_forget, tp_rank * unit_count, unit_count, 0)
    local_output = lax.dynamic_slice_in_dim(basis_output, tp_rank * unit_count, unit_count, 0)
    coords_forget = jnp.dot(gate_grad, local_forget, preferred_element_type=jnp.float32)
    coords_output = jnp.dot(head_out, local_output, preferred_element_type=jnp.float32)
    coords_forget, coords_output = lax.psum((coords_forget, coords_output), "tp")
    part_forget = split_product(coords_forget, hidden_in)
    part_output = split_product(coords_output, out_cot)
    proj = lax.psum_scatter(
        jnp.concatenate([part_forget, part_output], axis=1), "fs", scatter_dimension=0, tiled=True
    )
    mean_f, var_f, dir_forget = moment_update(mean_forget, var_forget, proj[:, :feat_cols])
    mean_o, var_o, dir_output = moment_update(mean_output, var_output, proj[:, feat_cols:])
    dir_forget, dir_output = (
        lax.all_gather(dir_forget, "fs", axis=0, tiled=True),
        lax.all_gather(dir_output, "fs", axis=0, tiled=True),
    )
    upd_forget = jnp.dot(rows_forget, dir_forget, precision=highest)
    upd_output = jnp.dot(rows_output, dir_output, precision=highest)
    total = float(basis_forget.shape[0] * feat_cols * lax.axis_size("tp"))
    sum_forget, sum_output = lax.psum(
        (jnp.sum(upd_forget * upd_forget), jnp.sum(upd_output * upd_output)), ("fs", "tp")
    )
    step_forget = upd_forget * lax.rsqrt(sum_forget / total + norm_eps)
    step_output = (upd_output * lax.rsqrt(sum_output / total + norm_eps)).T
    new_forget = weight_forget - step_rate * step_forget
    new_output = weight_output - step_rate * step_output
    copy_forget, copy_output = (
        lax.all_gather(new_forget.astype(jnp.bfloat16), "fs", axis=0, tiled=True),
        lax.all_gather(new_output.astype(jnp.bfloat16), "fs", axis=1, tiled=True),
    )
    return (
        step_forget,
        step_output,
        new_forget,
        new_output,
        mean_f,
        var_f,
        mean_o,
        var_o,
        copy_forget,
        copy_output,
    )


def fits(n_fs, n_tp, forget_pre, hidden_in, basis):
    tokens, units = forget_pre.shape
    quarter = tokens // n_tp
    part = basis.shape[1] // n_fs
    return (
        n_tp % CORES == 0
        and n_tp > CORES
        and n_fs > 1
        and tokens % n_tp == 0
        and units % LANES == 0
        and hidden_in.shape[1] % LANES == 0
        and quarter % (2 * SUBLANES) == 0
        and part % (2 * SUBLANES) == 0
    )


def device_step(n_fs, n_tp, *args):
    if fits(n_fs, n_tp, args[1], args[0], args[6]):
        return kernels_device(n_fs, n_tp, *args)
    return per_device(*args)


def solution(mesh):
    return jax.shard_map(
        functools.partial(device_step, mesh.shape["fs"], mesh.shape["tp"]),
        mesh=mesh,
        in_specs=(
            P("fs", "tp"),
            P("fs", "tp"),
            P("fs", "tp"),
            P("tp"),
            P("fs", "tp"),
            P("fs", "tp"),
            P(),
            P(),
            P("fs", "tp"),
            P("tp", "fs"),
            P("fs", "tp"),
            P("fs", "tp"),
            P("fs", "tp"),
            P("fs", "tp"),
        ),
        out_specs=(
            P("fs", "tp"),
            P("tp", "fs"),
            P("fs", "tp"),
            P("tp", "fs"),
            P("fs", "tp"),
            P("fs", "tp"),
            P("fs", "tp"),
            P("fs", "tp"),
            P(None, "tp"),
            P("tp", None),
        ),
        check_vma=False,
    )
```
